32 devices in a mesh: sp: 4 (over y, x), dp: 8 (over z, core).
Axes of the slice: x: 2, y: 2, z: 4, core: 2. Of those that a mesh axis runs over, the one named last changes fastest.
Arguments:
- tokens: bfloat16 [8, 768, 4096], P('dp', 'sp'), may hold values from -30 to 30
- query_weight: bfloat16 [4096, 512], P('dp', 'sp'), may hold values from -0.09375 to 0.09375
- key_weight: bfloat16 [4096, 512], P('dp', 'sp'), may hold values from -0.09375 to 0.09375
- value_weight: bfloat16 [4096, 512], P('dp', 'sp'), may hold values from -0.09375 to 0.09375
- cum_gate: float32 [8, 4, 768], P('dp', 'sp'), may hold values from -3072 to 0, as said below
Outputs:
- attended: bfloat16 [8, 768, 512], P('dp', 'sp')
The draws below stay inside these ranges and needn't reach their ends.
Inputs may be any that keep to these rules, and one draw needn't show every extreme that they name: `cum_gate`: never rising along positions; the first position holds one step's log gate.
All inputs are finite; a program needn't handle non-finite values.
Results may differ from the reference program's by a relative error of at most 0.0076.
The reference program's roundings to bfloat16 on the way count: a program that leaves them out, or rounds other values in their place, can miss the bound.
Values may be sent and summed in bfloat16 or wider, within the bound.
A program may use at most 128 MiB of HBM per device.

```python
import jax
import jax.numpy as jnp
from jax import lax

D = 4096
HEAD = 128
TOK_DEV = 192
HEADS = 4
WIDTH = 512
LEN = 768
SEQS = 8


def draw_tokens(key, part):
    base = jnp.clip(jax.random.normal(jax.random.fold_in(key, 11), (SEQS, LEN, D), jnp.float32), -6.0, 6.0)
    return base.astype(jnp.bfloat16)


def shared_matrix(key):
    return jax.random.normal(jax.random.fold_in(key, 21), (D, WIDTH), jnp.float32)


def draw_query_weight(key, part):
    return (jnp.clip(shared_matrix(key), -6.0, 6.0) / 64.0).astype(jnp.bfloat16)


def draw_key_weight(key, part):
    other = jax.random.normal(jax.random.fold_in(key, 22), (D, WIDTH), jnp.float32)
    return (jnp.clip(other, -6.0, 6.0) / 64.0).astype(jnp.bfloat16)


def draw_cum_gate(key, part):
    order = jax.random.permutation(jax.random.fold_in(key, 31), HEADS)
    slow = order < HEADS // 2
    rate = jnp.where(slow, 1.0 / LEN, 1.0 / 40.0)
    blocks = LEN // TOK_DEV
    block_factor = jnp.exp(jax.random.uniform(jax.random.fold_in(key, 32), (SEQS, HEADS, blocks, 1), jnp.float32, -0.69, 0.69))
    block_factor = jnp.broadcast_to(block_factor, (SEQS, HEADS, blocks, TOK_DEV)).reshape(SEQS, HEADS, LEN)
    step_factor = jax.random.uniform(jax.random.fold_in(key, 33), (SEQS, HEADS, LEN), jnp.float32, 0.2, 1.8)
    log_gate = -rate[None, :, None] * block_factor * step_factor
    return jnp.cumsum(log_gate, axis=2).astype(jnp.float32)


def block_scale(own_key, shape, shards, least, top_value):
    gain = 1.0
    for axis_at, shards_of in shards:
        steps = jax.random.uniform(jax.random.fold_in(jax.random.fold_in(own_key, 6), axis_at), (shards_of,), jnp.float32, least / len(shards), top_value / len(shards))
        gain = gain * jnp.repeat(jnp.exp(steps), shape[axis_at] // shards_of).reshape((-1,) + (1,) * (len(shape) - 1 - axis_at))
    return gain


def centred(key, shape, deviation, bound, cuts=(), dtype=jnp.bfloat16):
    values = deviation * jax.random.normal(key, shape, jnp.float32)
    if cuts:
        values = values * block_scale(key, shape, cuts, -0.22, 0.18)
    return jnp.clip(values, -bound, bound).astype(dtype)


def setup_inputs(seed: int = 0) -> dict:
    seeds = jax.random.split(jax.random.key(seed), 6)
    tokens = draw_tokens(jax.random.fold_in(seeds[5], 71), 0)
    query_weight = draw_query_weight(jax.random.fold_in(seeds[5], 71), 0)
    key_weight = draw_key_weight(jax.random.fold_in(seeds[5], 71), 0)
    value_weight = centred(seeds[3], (D, WIDTH), D ** -0.5, 0.09375, ((0, 8), (1, 4)))
    cum_gate = draw_cum_gate(jax.random.fold_in(seeds[5], 71), 0)
    return {"tokens": tokens, "query_weight": query_weight, "key_weight": key_weight, "value_weight": value_weight, "cum_gate": cum_gate}


block_rows = 512


def attend(queries, keys, values, gates):
    length = queries.shape[0]
    scale = queries.shape[1] ** -0.5
    pieces = []
    for start in range(0, length, block_rows):
        finish = min(start + block_rows, length)
        scores = jnp.dot(queries[start:finish], keys[:finish].T, preferred_element_type=jnp.float32) * scale
        scores = scores + gates[start:finish, None] - gates[None, :finish]
        rows_at = start + lax.broadcasted_iota(jnp.int32, scores.shape, 0)
        cols_at = lax.broadcasted_iota(jnp.int32, scores.shape, 1)
        scores = jnp.where(cols_at <= rows_at, scores, -1e30)
        top = jnp.max(scores, axis=1, keepdims=True)
        weights = jnp.exp(scores - top)
        total = jnp.sum(weights, axis=1, keepdims=True)
        summed = jnp.dot(weights.astype(jnp.bfloat16), values[:finish], preferred_element_type=jnp.float32)
        pieces.append((summed / total).astype(jnp.bfloat16))
    return jnp.concatenate(pieces, axis=0)


def reference(tokens, query_weight, key_weight, value_weight, cum_gate):
    def one_sequence(inputs):
        rows, gates = inputs
        queries = jnp.dot(rows, query_weight, preferred_element_type=jnp.float32).astype(jnp.bfloat16)
        keys = jnp.dot(rows, key_weight, preferred_element_type=jnp.float32).astype(jnp.bfloat16)
        values = jnp.dot(rows, value_weight, preferred_element_type=jnp.float32).astype(jnp.bfloat16)

        def by_head(array):
            return jnp.transpose(array.reshape(LEN, HEADS, HEAD), (1, 0, 2))

        heads_out = lax.map(lambda group: attend(group[0], group[1], group[2], group[3]),
                            (by_head(queries), by_head(keys), by_head(values), gates))
        return jnp.transpose(heads_out, (1, 0, 2)).reshape(LEN, HEADS * HEAD)

    return lax.map(one_sequence, (tokens, cum_gate))
```

```python
import functools
import math

import jax
import jax.numpy as jnp
from jax import lax
from jax.experimental import pallas as pl
from jax.experimental.pallas import tpu as pltpu
from jax.sharding import PartitionSpec as P

MESH = pl.DeviceIdType.MESH
block_rows = 256


def kernel(
    nx, ny, nz, cores, split, sub, early,
    tok_hbm, wq_hbm, wk_hbm, wv_hbm, gate_ref, out_ref,
    xbuf, wbuf, acc, qkv, qout, gcol, attn, obuf,
    lsem, tsem, xsend, xrecv, wrecv, precv, upsem, downsem, sideq, sidesem, psem,
    qsend, qrecv, osend, orecv,
):
    tok, depth = tok_hbm.shape
    rows, head = wq_hbm.shape
    pieces = rows // sub
    chunk = cores * rows
    group = nx * tok
    length = ny * group
    s, d = lax.axis_index("sp"), lax.axis_index("dp")
    y, x = s // nx, s % nx
    z, c = d // cores, d % cores
    others = [(y + k) % ny for k in range(1, ny)]
    early_rows = pl.ds(0, early * sub)
    late_rows = pl.ds(early * sub, rows - early * sub)
    parts = (pl.ds(0, split), pl.ds(split, tok - split))

    def columns(zb):
        return pl.ds(pl.multiple_of(zb * chunk, chunk), chunk)

    low = jnp.minimum(z, nz - 1 - z)

    def nearest(k):
        if k == 0:
            return z
        near = z - (k + 1) // 2 if k % 2 else z + k // 2
        far = jnp.where(z < nz - 1 - z, z + k - low, z - k + low)
        return jnp.where(k <= 2 * low, near, far)

    loads = [
        pltpu.make_async_copy(ref, wbuf.at[y, d, :, pl.ds(i * head, head)], lsem.at[i])
        for i, ref in enumerate((wq_hbm, wk_hbm, wv_hbm))
    ]
    own_load = pltpu.make_async_copy(tok_hbm, xbuf.at[x], tsem)
    for load in loads:
        load.start()
    own_load.start()

    barrier = pltpu.get_barrier_semaphore()
    for k in range(1, nx * ny):
        pl.semaphore_signal(
            barrier, inc=1, device_id={"sp": (s + k) % (nx * ny)}, device_id_type=MESH
        )
    above = {"dp": jnp.minimum(z + 1, nz - 1) * cores + c}
    below = {"dp": jnp.maximum(z - 1, 0) * cores + c}
    beside = {"dp": z * cores + 1 - c}

    @pl.when(z < nz - 1)
    def _():
        pl.semaphore_signal(barrier, inc=1, device_id=above, device_id_type=MESH)

    @pl.when(z > 0)
    def _():
        pl.semaphore_signal(barrier, inc=1, device_id=below, device_id_type=MESH)

    if cores > 1:
        pl.semaphore_signal(barrier, inc=1, device_id=beside, device_id_type=MESH)
    inner = (z > 0) & (z < nz - 1)
    ends = jnp.where(inner, 2, 1) if nz > 1 else 0
    pl.semaphore_wait(barrier, nx * ny - 1 + cores - 1 + ends)

    def aside(k):
        return {"sp": ((y + k) % ny) * nx + x}

    def send_tokens(j, zb, g):
        return pltpu.make_async_remote_copy(
            src_ref=tok_hbm.at[parts[g], columns(zb)],
            dst_ref=xbuf.at[x, parts[g], columns(zb)],
            send_sem=xsend.at[j - 1, zb, g], recv_sem=xrecv.at[x, zb, g],
            device_id={"sp": y * nx + (x + j) % nx}, device_id_type=MESH,
        )

    def tokens_here(zb, g):
        for j in range(1, nx):
            i = (x + j) % nx
            pltpu.make_async_remote_copy(
                src_ref=tok_hbm.at[parts[g], columns(zb)],
                dst_ref=xbuf.at[i, parts[g], columns(zb)],
                send_sem=xsend.at[j - 1, zb, g], recv_sem=xrecv.at[i, zb, g],
                device_id={"sp": y * nx + i}, device_id_type=MESH,
            ).wait_recv()

    def piece(p):
        return pl.ds(pl.multiple_of(p * sub, sub), sub)

    def copy_block(h, at, part, send_sem, recv_sem, device):
        ref = wbuf.at[h, at, part]
        return pltpu.make_async_remote_copy(
            src_ref=ref, dst_ref=ref, send_sem=send_sem, recv_sem=recv_sem,
            device_id=device, device_id_type=MESH,
        )

    def up(h, zb, part, p):
        return copy_block(h, zb * cores + c, part, upsem.at[h, zb], wrecv.at[h, zb, p], above)

    def down(h, zb, part, p):
        return copy_block(h, zb * cores + c, part, downsem.at[h, zb], wrecv.at[h, zb, p], below)

    def side_early(k, p):
        return copy_block(y, d, piece(p), sideq.at[k - 1], wrecv.at[y, z, p], aside(k))

    def side(k, zb, part):
        return copy_block(
            y, zb * cores + c, part, sidesem.at[k - 1, zb], wrecv.at[y, zb, early], aside(k)
        )

    def pair(h, zb, which, core):
        part = early_rows if which else late_rows
        return copy_block(
            h, zb * cores + core, part, psem.at[h, zb, which], precv.at[h, zb, which], beside
        )

    def arrived(h, zb, part, p):
        copy_block(
            h, zb * cores + c, part, lsem.at[0], wrecv.at[h, zb, p], aside(1)
        ).wait_recv()

    def share(h, zb, which):
        if cores > 1:
            pair(h, zb, which, c).start()

    def shared(h, zb):
        if cores > 1:
            for which in range(2):
                pair(h, zb, which, 1 - c).wait_recv()

    def both_ways(h, zb, p):
        pl.when(z < nz - 1)(lambda: up(h, zb, piece(p), p).start())
        pl.when(z > 0)(lambda: down(h, zb, piece(p), p).start())

    def pass_on(h, zb, p, rising):
        if rising:
            pl.when(z < nz - 1)(lambda: up(h, zb, piece(p), p).start())
        else:
            pl.when(z > 0)(lambda: down(h, zb, piece(p), p).start())

    def each(t, act):
        pl.when(z - t >= 0)(lambda: act(z - t, True))
        pl.when(z + t < nz)(lambda: act(z + t, False))

    def loop(first, last, act):
        def step(p, carry):
            act(p)
            return carry

        lax.fori_loop(first, last, step, 0)

    def relay_own(t, crosses):
        def take(p):
            def one(zb, rising):
                arrived(y, zb, piece(p), p)
                pass_on(y, zb, p, rising)
                if crosses:
                    for k in range(1, ny):
                        side(k, zb, piece(p)).start()

            each(t, one)

        loop(early if crosses else 0, pieces if crosses else early, take)
        each(t, lambda zb, rising: share(y, zb, 0 if crosses else 1))

    def relay_other(t):
        def take(p):
            for h in others:
                if t == 0:
                    arrived(h, z, piece(p), p)
                    both_ways(h, z, p)
                    continue

                def one(zb, rising, h=h):
                    arrived(h, zb, piece(p), p)
                    pass_on(h, zb, p, rising)

                each(t, one)

        loop(0, early, take)
        for h in others:
            if t == 0:
                share(h, z, 1)
            else:
                each(t, lambda zb, rising, h=h: share(h, zb, 1))

    for k in range(nz):
        for j in range(1, nx):
            send_tokens(j, nearest(k), 0).start()
    for k in range(nz):
        for j in range(1, nx):
            send_tokens(j, nearest(k), 1).start()
    for load in loads:
        load.wait()
    loop(0, early, lambda p: [side_early(k, p).start() for k in range(1, ny)] and None)
    loop(early, pieces, lambda p: both_ways(y, z, p))
    for k in range(1, ny):
        side(k, z, late_rows).start()
    share(y, z, 0)
    share(y, z, 1)

    for start in range(0, length, 128):
        row = gate_ref[:, start : start + 128]
        gcol[start : start + 128, :] = jnp.broadcast_to(row, (128, 128)).T
    acc[...] = jnp.zeros_like(acc)
    own_load.wait()

    def add(h, zb, i, part):
        weights = wbuf[h, pl.ds(zb * cores, cores)].reshape(chunk, 3 * head)
        acc[h, i, part, :] += jnp.dot(
            xbuf[i, part, columns(zb)], weights, preferred_element_type=jnp.float32
        )

    everything = pl.ds(0, tok)

    def add_others(k):
        zb = nearest(k)
        for h in others:
            arrived(h, zb, late_rows, early)
            share(h, zb, 0)
        for h in others:
            shared(h, zb)
            add(h, zb, x, everything)
        tokens_here(zb, 0)
        for h in others:
            for j in range(1, nx):
                add(h, zb, (x + j) % nx, parts[0])

    def add_last_rows(k):
        zb = nearest(k)
        tokens_here(zb, 1)
        for h in others:
            for j in range(1, nx):
                add(h, zb, (x + j) % nx, parts[1])

    def add_own(k):
        zb = nearest(k)
        if k > 0:

            @pl.when(jnp.logical_not(inner))
            def _():
                loop(0, early, lambda p: arrived(y, zb, piece(p), p))
                share(y, zb, 1)

        shared(y, zb)
        for i in range(nx):
            add(y, zb, i, everything)

    def own_rows(i, g):
        at = y * group + i * tok + (split if g else 0)
        return pl.ds(pl.multiple_of(at, 16), parts[g].size)

    def send_qkv(k, i, g):
        return pltpu.make_async_remote_copy(
            src_ref=qout.at[k - 1, i, parts[g]], dst_ref=qkv.at[own_rows(i, g)],
            send_sem=qsend.at[k - 1, i, g], recv_sem=qrecv.at[y, i, g],
            device_id=aside(k), device_id_type=MESH,
        )

    def swap(i, g):
        for k in range(1, ny):
            qout[k - 1, i, parts[g], :] = acc[others[k - 1], i, parts[g], :].astype(jnp.bfloat16)
            send_qkv(k, i, g).start()

    for t in range(1, nz):
        relay_own(t, True)
        relay_other(t - 1)
        if t == 1:

            @pl.when(jnp.logical_not(inner))
            def _():
                loop(0, early, lambda p: both_ways(y, z, p))

        if t > 1:
            add_others(t - 2)
    relay_other(nz - 1)

    @pl.when(inner)
    def _():
        loop(0, early, lambda p: both_ways(y, z, p))
        relay_own(1, False)

    for k in range(max(nz - 2, 0), nz):
        add_others(k)
    for g in range(2):
        swap(x, g)
    for j in range(1, nx):
        swap((x + j) % nx, 0)

    @pl.when(inner)
    def _():
        for t in range(2, nz):
            relay_own(t, False)

    add_last_rows(0)
    add_own(0)
    if nz > 1:
        add_last_rows(1)
        add_own(1)
    for k in range(2, nz):
        add_last_rows(k)
    for j in range(1, nx):
        swap((x + j) % nx, 1)
    for k in range(2, nz):
        add_own(k)
    for i in range(nx):
        for g in range(2):
            qkv[own_rows(i, g), :] = acc[y, i, parts[g], :].astype(jnp.bfloat16)
    for k in range(1, ny):
        other = (y + k) % ny
        for i in range(nx):
            for g in range(2):
                at = other * group + i * tok + (split if g else 0)
                taken = pl.ds(pl.multiple_of(at, 16), parts[g].size)
                pltpu.make_async_remote_copy(
                    src_ref=qout.at[k - 1, i, parts[g]], dst_ref=qkv.at[taken],
                    send_sem=qsend.at[k - 1, i, g], recv_sem=qrecv.at[other, i, g],
                    device_id={"sp": other * nx + x}, device_id_type=MESH,
                ).wait_recv()

    def send_out(to):
        return pltpu.make_async_remote_copy(
            src_ref=attn.at[pl.ds(to * tok, tok)],
            dst_ref=obuf.at[:, pl.ds(pl.multiple_of(s * head, head), head)],
            send_sem=osend.at[to], recv_sem=orecv.at[s],
            device_id={"sp": to}, device_id_type=MESH,
        )

    scale = head ** (-0.5)
    sent = 0
    for start in range(0, length, block_rows):
        finish = min(start + block_rows, length)
        scores = (
            lax.dot_general(
                qkv[start:finish, :head], qkv[:finish, head : 2 * head],
                (((1,), (1,)), ((), ())), preferred_element_type=jnp.float32,
            )
            * scale
        )
        scores = scores + gcol[start:finish, :1] - gate_ref[:, :finish]
        rows_at = start + lax.broadcasted_iota(jnp.int32, scores.shape, 0)
        cols_at = lax.broadcasted_iota(jnp.int32, scores.shape, 1)
        scores = jnp.where(cols_at <= rows_at, scores, -1e30)
        top = jnp.max(scores, axis=1, keepdims=True)
        weights = jnp.exp(scores - top)
        total = jnp.sum(weights, axis=1, keepdims=True)
        summed = jnp.dot(
            weights.astype(jnp.bfloat16), qkv[:finish, 2 * head :],
            preferred_element_type=jnp.float32,
        )
        attn[start:finish, :] = (summed / total).astype(jnp.bfloat16)
        while (sent + 1) * tok <= finish:

            @pl.when(s != sent)
            def _(to=sent):
                send_out(to).start()

            @pl.when(s == sent)
            def _(to=sent):
                obuf[:, pl.ds(pl.multiple_of(s * head, head), head)] = attn[
                    to * tok : (to + 1) * tok, :
                ]

            sent += 1

    for k in range(1, nx * ny):
        source = (s + k) % (nx * ny)
        pltpu.make_async_remote_copy(
            src_ref=attn.at[pl.ds(0, tok)],
            dst_ref=obuf.at[:, pl.ds(pl.multiple_of(source * head, head), head)],
            send_sem=osend.at[source], recv_sem=orecv.at[source],
            device_id={"sp": source}, device_id_type=MESH,
        ).wait_recv()
    last = pltpu.make_async_copy(obuf, out_ref, lsem.at[0])
    last.start()

    for zb in range(nz):
        for j in range(1, nx):
            for g in range(2):
                send_tokens(j, zb, g).wait_send()
        upward = (z < nz - 1) & (zb <= z)
        downward = (z > 0) & (zb >= z)
        whole = pl.ds(0, rows)
        for h, part in [(y, whole)] + [(h, early_rows) for h in others]:
            pl.when(upward)(lambda: up(h, zb, part, 0).wait_send())
            pl.when(downward)(lambda: down(h, zb, part, 0).wait_send())
            if cores > 1:
                for which in range(2):
                    pair(h, zb, which, c).wait_send()
        for k in range(1, ny):
            side(k, zb, late_rows).wait_send()
    for k in range(1, ny):
        copy_block(y, d, early_rows, sideq.at[k - 1], wrecv.at[y, z, 0], aside(k)).wait_send()
    for k in range(1, ny):
        for i in range(nx):
            for g in range(2):
                send_qkv(k, i, g).wait_send()
    for to in range(nx * ny):
        pl.when(s != to)(lambda to=to: send_out(to).wait_send())
    last.wait()


def body(sp, dp, tokens, query_weight, key_weight, value_weight, cum_gate):
    nx = max(n for n in range(1, math.isqrt(sp) + 1) if sp % n == 0)
    ny = sp // nx
    cores = 2 if dp % 2 == 0 else 1
    nz = dp // cores
    tok, depth = tokens.shape[1:]
    rows, head = query_weight.shape
    length = sp * tok
    split = tok * 3 // 4 // 16 * 16
    sub = min(64, rows // 4)
    early = max(rows // sub * 3 // 8, 1)
    dma = pltpu.SemaphoreType.DMA
    anywhere = pl.BlockSpec(memory_space=pl.ANY)
    vmem = pl.BlockSpec(memory_space=pltpu.VMEM)
    out = pl.pallas_call(
        functools.partial(kernel, nx, ny, nz, cores, split, sub, early),
        out_shape=jax.ShapeDtypeStruct((tok, sp * head), jnp.bfloat16),
        in_specs=[anywhere] * 4 + [vmem],
        out_specs=anywhere,
        scratch_shapes=[
            pltpu.VMEM((nx, tok, depth), jnp.bfloat16),
            pltpu.VMEM((ny, dp, rows, 3 * head), jnp.bfloat16),
            pltpu.VMEM((ny, nx, tok, 3 * head), jnp.float32),
            pltpu.VMEM((length, 3 * head), jnp.bfloat16),
            pltpu.VMEM((ny - 1, nx, tok, 3 * head), jnp.bfloat16),
            pltpu.VMEM((length, 128), jnp.float32),
            pltpu.VMEM((length, head), jnp.bfloat16),
            pltpu.VMEM((tok, sp * head), jnp.bfloat16),
            dma((3,)),
            dma,
            dma((nx - 1, nz, 2)),
            dma((nx, nz, 2)),
            dma((ny, nz, rows // sub)),
            dma((ny, nz, 2)),
            dma((ny, nz)),
            dma((ny, nz)),
            dma((ny - 1,)),
            dma((ny - 1, nz)),
            dma((ny, nz, 2)),
            dma((ny - 1, nx, 2)),
            dma((ny, nx, 2)),
            dma((sp,)),
            dma((sp,)),
        ],
        compiler_params=pltpu.CompilerParams(
            collective_id=0, has_side_effects=True, vmem_limit_bytes=60 * 1024 * 1024
        ),
    )(tokens[0], query_weight, key_weight, value_weight, cum_gate[0])
    return out[None]


def solution(mesh):
    in_specs = (
        P("dp", "sp", None),
        P("dp", "sp"),
        P("dp", "sp"),
        P("dp", "sp"),
        P("dp", "sp", None),
    )
    out_specs = P("dp", "sp", None)
    return jax.shard_map(
        functools.partial(body, mesh.shape["sp"], mesh.shape["dp"]),
        mesh=mesh, in_specs=in_specs, out_specs=out_specs, check_vma=False,
    )
```

```python
import functools
import math

import jax
import jax.numpy as jnp
from jax import lax
from jax.experimental import pallas as pl
from jax.experimental.pallas import tpu as pltpu
from jax.sharding import PartitionSpec as P

MESH = pl.DeviceIdType.MESH


def kernel(
    nx, ny, nz, cores, split, early, cuts, kept,
    tok_hbm, wq_hbm, wk_hbm, wv_hbm, gate_hbm, out_ref,
    xbuf, wbuf, acc, qkv, qout, gate_ref, gcol, attn, bias,
    lsem, tsem, gsem, xsend, xrecv, ownrecv, farrecv, precv, zsend, sideq, sidesem, psem,
    qsend, qrecv, osend, orecv,
):
    tok, depth = tok_hbm.shape
    rows, head = wq_hbm.shape
    chunk = cores * rows
    group = nx * tok
    length = ny * group
    s, d = lax.axis_index("sp"), lax.axis_index("dp")
    y, x = s // nx, s % nx
    z, c = d // cores, d % cores
    others = [(y + k) % ny for k in range(1, ny)]
    early_rows = pl.ds(0, early)
    late_rows = pl.ds(early, rows - early)
    whole = pl.ds(0, rows)
    parts = (pl.ds(0, split), pl.ds(split, tok - split))

    def columns(zb):
        return pl.ds(pl.multiple_of(zb * chunk, chunk), chunk)

    low = jnp.minimum(z, nz - 1 - z)

    def nearest(k):
        if k == 0:
            return z
        near = z - (k + 1) // 2 if k % 2 else z + k // 2
        far = jnp.where(z < nz - 1 - z, z + k - low, z - k + low)
        return jnp.where(k <= 2 * low, near, far)

    loads = [
        pltpu.make_async_copy(ref, wbuf.at[y, z, c, :, pl.ds(i * head, head)], lsem)
        for i, ref in enumerate((wq_hbm, wk_hbm, wv_hbm))
    ]
    own_load = pltpu.make_async_copy(tok_hbm, xbuf.at[x], tsem)
    for load in loads:
        load.start()
    own_load.start()
    gate_load = pltpu.make_async_copy(gate_hbm, gate_ref, gsem)
    gate_load.start()

    barrier = pltpu.get_barrier_semaphore()
    peers = [y * nx + (x + j) % nx for j in range(1, nx)]
    peers += [((y + k) % ny) * nx + x for k in range(1, ny)]
    for peer in peers:
        pl.semaphore_signal(barrier, inc=1, device_id={"sp": peer}, device_id_type=MESH)
    above = {"dp": jnp.minimum(z + 1, nz - 1) * cores + c}
    below = {"dp": jnp.maximum(z - 1, 0) * cores + c}
    beside = {"dp": z * cores + 1 - c}

    @pl.when(z < nz - 1)
    def _():
        pl.semaphore_signal(barrier, inc=1, device_id=above, device_id_type=MESH)

    @pl.when(z > 0)
    def _():
        pl.semaphore_signal(barrier, inc=1, device_id=below, device_id_type=MESH)

    if cores > 1:
        pl.semaphore_signal(barrier, inc=1, device_id=beside, device_id_type=MESH)
    inner = (z > 0) & (z < nz - 1)
    levels = jnp.where(inner, 2, 1) if nz > 1 else 0
    pl.semaphore_wait(barrier, len(peers) + cores - 1 + levels)

    def aside(k):
        return {"sp": ((y + k) % ny) * nx + x}

    def send_tokens(j, zb, g):
        return pltpu.make_async_remote_copy(
            src_ref=tok_hbm.at[parts[g], columns(zb)],
            dst_ref=xbuf.at[x, parts[g], columns(zb)],
            send_sem=xsend.at[j - 1], recv_sem=xrecv.at[j - 1, zb, g],
            device_id={"sp": y * nx + (x + j) % nx}, device_id_type=MESH,
        )

    def tokens_here(zb, g):
        for j in range(1, nx):
            i = (x - j + nx) % nx
            pltpu.make_async_remote_copy(
                src_ref=tok_hbm.at[parts[g], columns(zb)],
                dst_ref=xbuf.at[i, parts[g], columns(zb)],
                send_sem=xsend.at[j - 1], recv_sem=xrecv.at[j - 1, zb, g],
                device_id={"sp": y * nx + i}, device_id_type=MESH,
            ).wait_recv()

    def piece(which, p):
        size = early // cuts[1] if which else (rows - early) // cuts[0]
        return pl.ds(pl.multiple_of((0 if which else early) + p * size, 8), size)

    def mark(which, p):
        return p if which else cuts[1] + p

    def copy_block(h, zb, core, part, send_sem, recv_sem, device):
        ref = wbuf.at[h, zb, core, part]
        return pltpu.make_async_remote_copy(
            src_ref=ref, dst_ref=ref, send_sem=send_sem, recv_sem=recv_sem,
            device_id=device, device_id_type=MESH,
        )

    def landing(h, zb, p, place):
        for k in range(1, ny):
            if h is others[k - 1]:
                return farrecv.at[k - 1, zb, p]
        return ownrecv.at[place, p]

    def up(h, zb, part, p):
        return copy_block(h, zb, c, part, zsend.at[h, zb], landing(h, zb, p, zb), above)

    def down(h, zb, part, p):
        way = jnp.where(zb == z, nz, zb)
        return copy_block(
            h, zb, c, part, zsend.at[h, way], landing(h, zb, p, jnp.maximum(zb - 1, 0)), below
        )

    def side_early(k, p):
        return copy_block(
            y, z, c, piece(1, p), sideq.at[k - 1], farrecv.at[ny - k - 1, z, p], aside(k)
        )

    def side(k, zb, part):
        return copy_block(
            y, zb, c, part, sidesem.at[k - 1], farrecv.at[ny - k - 1, zb, cuts[1]], aside(k)
        )

    def pair(h, zb, part, core):
        return copy_block(h, zb, core, part, psem, precv.at[h, zb], beside)

    def arrived(h, zb, part, p):
        place = jnp.where(zb < z, zb, jnp.maximum(zb - 1, 0))
        copy_block(h, zb, c, part, lsem, landing(h, zb, p, place), aside(1)).wait_recv()

    def share(h, zb, which):
        if cores > 1:
            pair(h, zb, early_rows if which else late_rows, c).start()

    def shared(h, zb):
        if cores > 1:
            pair(h, zb, whole, 1 - c).wait_recv()

    def rise(h, zb, which, p):
        pl.when(z < nz - 1)(lambda: up(h, zb, piece(which, p), mark(which, p)).start())

    def sink(h, zb, which, p):
        pl.when(z > 0)(lambda: down(h, zb, piece(which, p), mark(which, p)).start())

    def both_ways(h, zb, which, p):
        rise(h, zb, which, p)
        sink(h, zb, which, p)

    def each(t, act):
        pl.when(z - t >= 0)(lambda: act(z - t, rise))
        pl.when(z + t < nz)(lambda: act(z + t, sink))

    def loop(which, act):
        def step(p, carry):
            act(p)
            return carry

        lax.fori_loop(0, cuts[which], step, 0)

    def relay_own(t):
        def take(p):
            def one(zb, onward):
                arrived(y, zb, piece(0, p), mark(0, p))
                onward(y, zb, 0, p)
                for k in range(1, ny):
                    side(k, zb, piece(0, p)).start()

            each(t, one)

        loop(0, take)
        each(t, lambda zb, onward: share(y, zb, 0))

    def relay_last(t, rising):
        zb, onward = (z - t, rise) if rising else (z + t, sink)

        @pl.when(zb >= 0 if rising else zb < nz)
        def _():
            def take(p):
                arrived(y, zb, piece(1, p), p)
                onward(y, zb, 1, p)

            loop(1, take)
            share(y, zb, 1)

    def finish_way(rising, steps):
        loop(1, lambda p: (rise if rising else sink)(y, z, 1, p))
        for t in range(1, steps + 1):
            relay_last(t, rising)

    def relay_other(t):
        def take(p):
            for h in others:
                if t == 0:
                    arrived(h, z, piece(1, p), p)
                    both_ways(h, z, 1, p)
                    continue

                def one(zb, onward, h=h):
                    arrived(h, zb, piece(1, p), p)
                    onward(h, zb, 1, p)

                each(t, one)

        loop(1, take)
        for h in others:
            if t == 0:
                share(h, z, 1)
            else:
                each(t, lambda zb, onward, h=h: share(h, zb, 1))

    for k in range(nz):
        for j in range(1, nx):
            send_tokens(j, nearest(k), 0).start()
    for k in range(nz):
        for j in range(1, nx):
            send_tokens(j, nearest(k), 1).start()
    pltpu.make_async_copy(wbuf.at[y, z, c], wbuf.at[y, z, c], lsem).wait()
    loop(1, lambda p: [side_early(k, p).start() for k in range(1, ny)] and None)
    loop(0, lambda p: both_ways(y, z, 0, p))
    for k in range(1, ny):
        side(k, z, late_rows).start()
    share(y, z, 0)
    share(y, z, 1)

    gate_load.wait()
    for start in range(0, length, 128):
        row = gate_ref[:, start : start + 128]
        gcol[start : start + 128, :] = jnp.broadcast_to(row, (128, 128)).T
    acc[...] = jnp.zeros_like(acc)
    log2e = math.log2(math.e)

    def bias_of(at, size, extent):
        gap = gcol[pl.ds(at, size), :1] - gate_ref[:, :extent]
        rows_at = at + lax.broadcasted_iota(jnp.int32, gap.shape, 0)
        cols_at = lax.broadcasted_iota(jnp.int32, gap.shape, 1)
        return jnp.where(cols_at <= rows_at, gap * log2e, -1e30)

    if kept:
        for r in range(ny):
            for i in range(nx):
                at, extent = (r * nx + i) * tok, (r + 1) * group
                bias[at : at + tok, :extent] = bias_of(at, tok, extent)
    own_load.wait()

    def add(h, zb, i, part):
        weights = wbuf[h, zb].reshape(chunk, 3 * head)
        acc[h, i, part, :] += jnp.dot(
            xbuf[i, part, columns(zb)], weights, preferred_element_type=jnp.float32
        )

    everything = pl.ds(0, tok)

    def own_rows(i, g):
        at = y * group + i * tok + (split if g else 0)
        return pl.ds(pl.multiple_of(at, 16), parts[g].size)

    def send_qkv(k, i, g):
        return pltpu.make_async_remote_copy(
            src_ref=qout.at[k - 1, i, parts[g]], dst_ref=qkv.at[own_rows(i, g)],
            send_sem=qsend.at[k - 1], recv_sem=qrecv.at[ny - k - 1],
            device_id=aside(k), device_id_type=MESH,
        )

    def swap(i, g):
        for k in range(1, ny):
            qout[k - 1, i, parts[g], :] = acc[others[k - 1], i, parts[g], :].astype(jnp.bfloat16)
            send_qkv(k, i, g).start()

    def take_side(k):
        for h in others:
            arrived(h, nearest(k), late_rows, cuts[1])
            share(h, nearest(k), 0)

    def add_others(k):
        zb = nearest(k)
        for h in others:
            shared(h, zb)
            add(h, zb, x, everything)
        if k == nz - 1:
            for g in range(2):
                swap(x, g)
        tokens_here(zb, 0)
        for h in others:
            for j in range(1, nx):
                add(h, zb, (x + j) % nx, parts[0])

    def add_last_rows(k):
        zb = nearest(k)
        tokens_here(zb, 1)
        for h in others:
            for j in range(1, nx):
                add(h, zb, (x + j) % nx, parts[1])

    def take_last(k):
        zb = nearest(k)

        @pl.when(jnp.logical_not(inner))
        def _():
            loop(1, lambda p: arrived(y, zb, piece(1, p), p))
            share(y, zb, 1)

    def add_own(k):
        zb = nearest(k)
        shared(y, zb)
        for i in range(nx):
            add(y, zb, i, everything)

    lower = z < nz - 1 - z
    for t in range(1, nz):
        relay_own(t)
        relay_other(t - 1)
        take_side(t - 1)
        if t == 1:

            @pl.when(jnp.logical_not(inner))
            def _():
                loop(1, lambda p: both_ways(y, z, 1, p))

        elif t - 1 <= (nz - 1) // 2:
            pl.when((low == t - 1) & lower)(lambda: finish_way(True, t - 1))
            pl.when((low == t - 1) & jnp.logical_not(lower))(lambda: finish_way(False, t - 1))
        if t > 1:
            add_others(t - 2)
    if nz > 1:
        add_others(nz - 2)
    pl.when(jnp.logical_not(inner))(lambda: take_side(nz - 1))
    relay_other(nz - 1)

    @pl.when(inner)
    def _():
        pl.when(lower)(lambda: finish_way(False, nz - 1))
        pl.when(jnp.logical_not(lower))(lambda: finish_way(True, nz - 1))
        take_side(nz - 1)

    add_others(nz - 1)
    for j in range(1, nx):
        swap((x + j) % nx, 0)

    add_last_rows(0)
    add_own(0)
    for k in range(1, nz):
        if k < nz - 1:
            take_last(k)
        add_last_rows(k)
    def send_out(to):
        return pltpu.make_async_remote_copy(
            src_ref=attn.at[pl.ds(pl.multiple_of(to * tok, tok), tok)],
            dst_ref=out_ref.at[:, pl.ds(pl.multiple_of(s * head, head), head)],
            send_sem=osend, recv_sem=orecv,
            device_id={"sp": to}, device_id_type=MESH,
        )

    scale = head ** (-0.5) * log2e

    def attend(r, i, extent):
        at = pl.multiple_of((r * nx + i) * tok, tok)
        scores = lax.dot_general(
            qkv[pl.ds(at, tok), :head], qkv[:extent, head : 2 * head],
            (((1,), (1,)), ((), ())), preferred_element_type=jnp.float32,
        )
        offset = bias[pl.ds(at, tok), :extent] if kept else bias_of(at, tok, extent)
        scores = scores * scale + offset
        top = jnp.max(scores, axis=1, keepdims=True)
        weights = jnp.exp2(scores - top)
        total = jnp.sum(weights, axis=1, keepdims=True)
        summed = jnp.dot(
            weights.astype(jnp.bfloat16), qkv[:extent, 2 * head :],
            preferred_element_type=jnp.float32,
        )
        attn[pl.ds(at, tok), :] = (summed / total).astype(jnp.bfloat16)

    def attend_beside(r):
        def step(j):
            i = (x + j) % nx
            attend(r, i, (r + 1) * group)
            send_out(r * nx + i).start()

        if nx > 2:
            lax.fori_loop(1, nx, lambda j, carry: (step(j), carry)[1], 0)
        else:
            for j in range(1, nx):
                step(j)

    def attend_far(r):
        attend_beside(r)
        attend(r, x, (r + 1) * group)
        send_out(r * nx + x).start()

    def attend_before(r):
        if nx > 2:
            attend_far(r)
            return
        for i in range(nx):
            attend(r, i, (r * nx + i + 1) * tok)
            send_out(r * nx + i).start()

    def swapped():
        for k in range(1, ny):
            other = (y + k) % ny
            taken = qkv.at[pl.ds(pl.multiple_of(other * group, group), group)]
            pltpu.make_async_remote_copy(
                src_ref=taken, dst_ref=taken, send_sem=qsend.at[k - 1],
                recv_sem=qrecv.at[k - 1], device_id=aside(k), device_id_type=MESH,
            ).wait_recv()

    for j in range(1, nx):
        swap((x + j) % nx, 1)
    if nz > 1:
        take_last(nz - 1)
    for k in range(1, nz - 1):
        add_own(k)

    @pl.when(y > 0)
    def _():
        swapped()
        for r in range(ny - 1):
            pl.when(r < y)(lambda r=r: attend_before(r))

    if nz > 1:
        add_own(nz - 1)
    for i in range(nx):
        for g in range(2):
            qkv[own_rows(i, g), :] = acc[y, i, parts[g], :].astype(jnp.bfloat16)

    @pl.when(y == 0)
    def _():
        attend_beside(0)
        swapped()

    for r in range(1, ny):
        pl.when(r > y)(lambda r=r: attend_far(r))
    for r in range(1, ny):
        pl.when(y == r)(lambda r=r: attend_beside(r))
    for r in range(ny):
        pl.when(y == r)(lambda r=r: attend(r, x, (r + 1) * group))
    out_ref[:, pl.ds(pl.multiple_of(s * head, head), head)] = attn[
        pl.ds(pl.multiple_of(s * tok, tok), tok), :
    ]

    for j in range(1, nx):
        pltpu.make_async_remote_copy(
            src_ref=tok_hbm, dst_ref=xbuf.at[x], send_sem=xsend.at[j - 1],
            recv_sem=xrecv.at[j - 1, 0, 0],
            device_id={"sp": y * nx + (x + j) % nx}, device_id_type=MESH,
        ).wait_send()
    for zb in range(nz):
        upward = (z < nz - 1) & (zb <= z)
        downward = (z > 0) & (zb >= z)
        for h, part in [(y, whole)] + [(h, early_rows) for h in others]:
            pl.when(upward)(lambda: up(h, zb, part, 0).wait_send())
            pl.when(downward)(lambda: down(h, zb, part, 0).wait_send())
    if cores > 1:
        sent = wbuf.at[:, :, c]
        pltpu.make_async_remote_copy(
            src_ref=sent, dst_ref=sent, send_sem=psem, recv_sem=precv.at[0, 0],
            device_id=beside, device_id_type=MESH,
        ).wait_send()
    for k in range(1, ny):
        copy_block(
            y, z, c, early_rows, sideq.at[k - 1], farrecv.at[ny - k - 1, z, 0], aside(k)
        ).wait_send()
        sent = wbuf.at[y, :, c, late_rows]
        pltpu.make_async_remote_copy(
            src_ref=sent, dst_ref=sent, send_sem=sidesem.at[k - 1],
            recv_sem=farrecv.at[ny - k - 1, z, 0], device_id=aside(k), device_id_type=MESH,
        ).wait_send()
        pltpu.make_async_remote_copy(
            src_ref=qout.at[k - 1], dst_ref=qout.at[k - 1], send_sem=qsend.at[k - 1],
            recv_sem=qrecv.at[k - 1], device_id=aside(k), device_id_type=MESH,
        ).wait_send()
    rest = attn.at[pl.ds(0, length - tok)]
    ends = pltpu.make_async_remote_copy(
        src_ref=rest, dst_ref=rest, send_sem=osend, recv_sem=orecv,
        device_id={"sp": (s + 1) % (nx * ny)}, device_id_type=MESH,
    )
    ends.wait_recv()
    ends.wait_send()


def body(sp, dp, tokens, query_weight, key_weight, value_weight, cum_gate):
    nx = max(n for n in range(1, math.isqrt(sp) + 1) if sp % n == 0)
    ny = sp // nx
    cores = 2 if dp % 2 == 0 else 1
    nz = dp // cores
    tok, depth = tokens.shape[1:]
    rows, head = query_weight.shape
    length = sp * tok
    split = tok * 5 // 6 // 16 * 16
    early = rows * 5 // 16
    kept = length * length * 4 <= 8 * 1024 * 1024
    cuts = max(rows // 256, 1), 1
    dma = pltpu.SemaphoreType.DMA
    hbm = pl.BlockSpec(memory_space=pltpu.HBM)
    vmem = pl.BlockSpec(memory_space=pltpu.VMEM)
    out = pl.pallas_call(
        functools.partial(kernel, nx, ny, nz, cores, split, early, cuts, kept),
        out_shape=pltpu.VMEM((tok, sp * head), jnp.bfloat16),
        in_specs=[hbm] * 5,
        out_specs=vmem,
        scratch_shapes=[
            pltpu.VMEM((nx, tok, depth), jnp.bfloat16),
            pltpu.VMEM((ny, nz, cores, rows, 3 * head), jnp.bfloat16),
            pltpu.VMEM((ny, nx, tok, 3 * head), jnp.float32),
            pltpu.VMEM((length, 3 * head), jnp.bfloat16),
            pltpu.VMEM((ny - 1, nx, tok, 3 * head), jnp.bfloat16),
            pltpu.VMEM((1, length), jnp.float32),
            pltpu.VMEM((length, 128), jnp.float32),
            pltpu.VMEM((length, head), jnp.bfloat16),
            pltpu.VMEM((length, length) if kept else (8, 128), jnp.float32),
            dma,
            dma,
            dma,
            dma((nx - 1,)),
            dma((nx - 1, nz, 2)),
            dma((max(nz - 1, 1), sum(cuts))),
            dma((ny - 1, nz, cuts[1] + 1)),
            dma((ny, nz)),
            dma((ny, nz + 1)),
            dma((ny - 1,)),
            dma((ny - 1,)),
            dma,
            dma((ny - 1,)),
            dma((ny - 1,)),
            dma,
            dma,
        ],
        compiler_params=pltpu.CompilerParams(
            collective_id=0, has_side_effects=True, vmem_limit_bytes=60 * 1024 * 1024
        ),
    )(tokens[0], query_weight, key_weight, value_weight, cum_gate[0])
    return out[None]


def solution(mesh):
    in_specs = (
        P("dp", "sp", None),
        P("dp", "sp"),
        P("dp", "sp"),
        P("dp", "sp"),
        P("dp", "sp", None),
    )
    out_specs = P("dp", "sp", None)
    return jax.shard_map(
        functools.partial(body, mesh.shape["sp"], mesh.shape["dp"]),
        mesh=mesh, in_specs=in_specs, out_specs=out_specs, check_vma=False,
    )
```

```python
import functools
import math

import jax
import jax.numpy as jnp
from jax import lax
from jax.experimental import pallas as pl
from jax.experimental.pallas import tpu as pltpu
from jax.sharding import PartitionSpec as P

MESH = pl.DeviceIdType.MESH


def kernel(
    nx, ny, nz, cores, split, early, cuts, kept,
    tok_hbm, wq_hbm, wk_hbm, wv_hbm, gate_hbm, out_ref,
    xbuf, wbuf, acc, qkv, qout, gate_ref, gcol, attn, bias,
    lsem, tsem, gsem, xsend, xrecv, ownrecv, farrecv, precv, zsend, sideq, sidesem, psem,
    qsend, qrecv, osend, orecv,
):
    tok, depth = tok_hbm.shape
    rows, head = wq_hbm.shape
    chunk = cores * rows
    group = nx * tok
    length = ny * group
    s, d = lax.axis_index("sp"), lax.axis_index("dp")
    y, x = s // nx, s % nx
    z, c = d // cores, d % cores
    others = [(y + k) % ny for k in range(1, ny)]
    early_rows = pl.ds(0, early)
    late_rows = pl.ds(early, rows - early)
    whole = pl.ds(0, rows)
    parts = (pl.ds(0, split), pl.ds(split, tok - split))

    def columns(zb):
        return pl.ds(pl.multiple_of(zb * chunk, chunk), chunk)

    low = jnp.minimum(z, nz - 1 - z)

    def nearest(k):
        if k == 0:
            return z
        near = z - (k + 1) // 2 if k % 2 else z + k // 2
        far = jnp.where(z < nz - 1 - z, z + k - low, z - k + low)
        return jnp.where(k <= 2 * low, near, far)

    loads = [
        pltpu.make_async_copy(ref, wbuf.at[y, z, c, :, pl.ds(i * head, head)], lsem)
        for i, ref in enumerate((wq_hbm, wk_hbm, wv_hbm))
    ]
    own_load = pltpu.make_async_copy(tok_hbm, xbuf.at[x], tsem)
    for load in loads:
        load.start()
    own_load.start()
    gate_load = pltpu.make_async_copy(gate_hbm, gate_ref, gsem)
    gate_load.start()

    barrier = pltpu.get_barrier_semaphore()
    peers = [y * nx + (x + j) % nx for j in range(1, nx)]
    peers += [((y + k) % ny) * nx + x for k in range(1, ny)]
    for peer in peers:
        pl.semaphore_signal(barrier, inc=1, device_id={"sp": peer}, device_id_type=MESH)
    above = {"dp": jnp.minimum(z + 1, nz - 1) * cores + c}
    below = {"dp": jnp.maximum(z - 1, 0) * cores + c}
    beside = {"dp": z * cores + 1 - c}

    @pl.when(z < nz - 1)
    def _():
        pl.semaphore_signal(barrier, inc=1, device_id=above, device_id_type=MESH)

    @pl.when(z > 0)
    def _():
        pl.semaphore_signal(barrier, inc=1, device_id=below, device_id_type=MESH)

    if cores > 1:
        pl.semaphore_signal(barrier, inc=1, device_id=beside, device_id_type=MESH)
    inner = (z > 0) & (z < nz - 1)
    levels = jnp.where(inner, 2, 1) if nz > 1 else 0
    pl.semaphore_wait(barrier, len(peers) + cores - 1 + levels)

    def aside(k):
        return {"sp": ((y + k) % ny) * nx + x}

    def send_tokens(j, zb, g):
        return pltpu.make_async_remote_copy(
            src_ref=tok_hbm.at[parts[g], columns(zb)],
            dst_ref=xbuf.at[x, parts[g], columns(zb)],
            send_sem=xsend.at[j - 1], recv_sem=xrecv.at[j - 1, zb, g],
            device_id={"sp": y * nx + (x + j) % nx}, device_id_type=MESH,
        )

    def tokens_here(zb, g):
        for j in range(1, nx):
            i = (x - j + nx) % nx
            pltpu.make_async_remote_copy(
                src_ref=tok_hbm.at[parts[g], columns(zb)],
                dst_ref=xbuf.at[i, parts[g], columns(zb)],
                send_sem=xsend.at[j - 1], recv_sem=xrecv.at[j - 1, zb, g],
                device_id={"sp": y * nx + i}, device_id_type=MESH,
            ).wait_recv()

    def piece(which, p):
        size = early // cuts[1] if which else (rows - early) // cuts[0]
        return pl.ds(pl.multiple_of((0 if which else early) + p * size, 8), size)

    def mark(which, p):
        return p if which else cuts[1] + p

    def copy_block(h, zb, core, part, send_sem, recv_sem, device):
        ref = wbuf.at[h, zb, core, part]
        return pltpu.make_async_remote_copy(
            src_ref=ref, dst_ref=ref, send_sem=send_sem, recv_sem=recv_sem,
            device_id=device, device_id_type=MESH,
        )

    def landing(h, zb, p, place):
        for k in range(1, ny):
            if h is others[k - 1]:
                return farrecv.at[k - 1, zb, p]
        return ownrecv.at[place, p]

    def up(h, zb, part, p):
        return copy_block(h, zb, c, part, zsend.at[h, zb], landing(h, zb, p, zb), above)

    def down(h, zb, part, p):
        way = jnp.where(zb == z, nz, zb)
        return copy_block(
            h, zb, c, part, zsend.at[h, way], landing(h, zb, p, jnp.maximum(zb - 1, 0)), below
        )

    def side_early(k, p):
        return copy_block(
            y, z, c, piece(1, p), sideq.at[k - 1], farrecv.at[ny - k - 1, z, p], aside(k)
        )

    def side(k, zb, part):
        return copy_block(
            y, zb, c, part, sidesem.at[k - 1], farrecv.at[ny - k - 1, zb, cuts[1]], aside(k)
        )

    def pair(h, zb, part, core):
        return copy_block(h, zb, core, part, psem, precv.at[h, zb], beside)

    def arrived(h, zb, part, p):
        place = jnp.where(zb < z, zb, jnp.maximum(zb - 1, 0))
        copy_block(h, zb, c, part, lsem, landing(h, zb, p, place), aside(1)).wait_recv()

    def share(h, zb, which):
        if cores > 1:
            pair(h, zb, early_rows if which else late_rows, c).start()

    def shared(h, zb):
        if cores > 1:
            pair(h, zb, whole, 1 - c).wait_recv()

    def rise(h, zb, which, p):
        pl.when(z < nz - 1)(lambda: up(h, zb, piece(which, p), mark(which, p)).start())

    def sink(h, zb, which, p):
        pl.when(z > 0)(lambda: down(h, zb, piece(which, p), mark(which, p)).start())

    def both_ways(h, zb, which, p):
        rise(h, zb, which, p)
        sink(h, zb, which, p)

    def each(t, act):
        pl.when(z - t >= 0)(lambda: act(z - t, rise))
        pl.when(z + t < nz)(lambda: act(z + t, sink))

    def loop(which, act):
        def step(p, carry):
            act(p)
            return carry

        lax.fori_loop(0, cuts[which], step, 0)

    def relay_own(t):
        def take(p):
            def one(zb, onward):
                arrived(y, zb, piece(0, p), mark(0, p))
                onward(y, zb, 0, p)
                for k in range(1, ny):
                    side(k, zb, piece(0, p)).start()

            each(t, one)

        loop(0, take)
        each(t, lambda zb, onward: share(y, zb, 0))

    def relay_last(t, rising):
        zb, onward = (z - t, rise) if rising else (z + t, sink)

        @pl.when(zb >= 0 if rising else zb < nz)
        def _():
            def take(p):
                arrived(y, zb, piece(1, p), p)
                onward(y, zb, 1, p)

            loop(1, take)
            share(y, zb, 1)

    def finish_way(rising, steps):
        loop(1, lambda p: (rise if rising else sink)(y, z, 1, p))
        for t in range(1, steps + 1):
            relay_last(t, rising)

    def relay_other(t):
        def take(p):
            for h in others:
                if t == 0:
                    arrived(h, z, piece(1, p), p)
                    both_ways(h, z, 1, p)
                    continue

                def one(zb, onward, h=h):
                    arrived(h, zb, piece(1, p), p)
                    onward(h, zb, 1, p)

                each(t, one)

        loop(1, take)
        for h in others:
            if t == 0:
                share(h, z, 1)
            else:
                each(t, lambda zb, onward, h=h: share(h, zb, 1))

    for k in range(nz):
        for j in range(1, nx):
            send_tokens(j, nearest(k), 0).start()
    for k in range(nz):
        for j in range(1, nx):
            send_tokens(j, nearest(k), 1).start()
    pltpu.make_async_copy(wbuf.at[y, z, c], wbuf.at[y, z, c], lsem).wait()
    loop(1, lambda p: [side_early(k, p).start() for k in range(1, ny)] and None)
    loop(0, lambda p: both_ways(y, z, 0, p))
    for k in range(1, ny):
        side(k, z, late_rows).start()
    share(y, z, 0)
    share(y, z, 1)

    gate_load.wait()
    for start in range(0, length, 128):
        row = gate_ref[:, start : start + 128]
        gcol[start : start + 128, :] = jnp.broadcast_to(row, (128, 128)).T
    acc[...] = jnp.zeros_like(acc)
    log2e = math.log2(math.e)

    def bias_of(at, size, extent):
        gap = gcol[pl.ds(at, size), :1] - gate_ref[:, :extent]
        rows_at = at + lax.broadcasted_iota(jnp.int32, gap.shape, 0)
        cols_at = lax.broadcasted_iota(jnp.int32, gap.shape, 1)
        return jnp.where(cols_at <= rows_at, gap * log2e, -1e30)

    if kept:
        for r in range(ny):
            for i in range(nx):
                at, extent = (r * nx + i) * tok, (r + 1) * group
                bias[at : at + tok, :extent] = bias_of(at, tok, extent)
    own_load.wait()

    def add(h, zb, i, part):
        weights = wbuf[h, zb].reshape(chunk, 3 * head)
        acc[h, i, part, :] += jnp.dot(
            xbuf[i, part, columns(zb)], weights, preferred_element_type=jnp.float32
        )

    everything = pl.ds(0, tok)

    def own_rows(i, g):
        at = y * group + i * tok + (split if g else 0)
        return pl.ds(pl.multiple_of(at, 16), parts[g].size)

    def send_qkv(k, i, g):
        return pltpu.make_async_remote_copy(
            src_ref=qout.at[k - 1, i, parts[g]], dst_ref=qkv.at[own_rows(i, g)],
            send_sem=qsend.at[k - 1], recv_sem=qrecv.at[ny - k - 1],
            device_id=aside(k), device_id_type=MESH,
        )

    def swap(i, g):
        for k in range(1, ny):
            qout[k - 1, i, parts[g], :] = acc[others[k - 1], i, parts[g], :].astype(jnp.bfloat16)
            send_qkv(k, i, g).start()

    def take_side(k):
        for h in others:
            arrived(h, nearest(k), late_rows, cuts[1])
            share(h, nearest(k), 0)

    def add_others(k):
        zb = nearest(k)
        for h in others:
            shared(h, zb)
            add(h, zb, x, everything)
        if k == nz - 1:
            for g in range(2):
                swap(x, g)
        tokens_here(zb, 0)
        for h in others:
            for j in range(1, nx):
                add(h, zb, (x + j) % nx, parts[0])

    def add_last_rows(k):
        zb = nearest(k)
        tokens_here(zb, 1)
        for h in others:
            for j in range(1, nx):
                add(h, zb, (x + j) % nx, parts[1])

    def take_last(k):
        zb = nearest(k)

        @pl.when(jnp.logical_not(inner))
        def _():
            loop(1, lambda p: arrived(y, zb, piece(1, p), p))
            share(y, zb, 1)

    def add_own(k):
        zb = nearest(k)
        shared(y, zb)
        for i in range(nx):
            add(y, zb, i, everything)

    lower = z < nz - 1 - z
    for t in range(1, nz):
        relay_own(t)
        relay_other(t - 1)
        take_side(t - 1)
        if t == 1:

            @pl.when(jnp.logical_not(inner))
            def _():
                loop(1, lambda p: both_ways(y, z, 1, p))

        elif t - 1 <= (nz - 1) // 2:
            pl.when((low == t - 1) & lower)(lambda: finish_way(True, t - 1))
            pl.when((low == t - 1) & jnp.logical_not(lower))(lambda: finish_way(False, t - 1))
        if t > 1:
            add_others(t - 2)
    if nz > 1:
        add_others(nz - 2)
    pl.when(jnp.logical_not(inner))(lambda: take_side(nz - 1))
    relay_other(nz - 1)

    @pl.when(inner)
    def _():
        pl.when(lower)(lambda: finish_way(False, nz - 1))
        pl.when(jnp.logical_not(lower))(lambda: finish_way(True, nz - 1))
        take_side(nz - 1)

    add_others(nz - 1)
    for j in range(1, nx):
        swap((x + j) % nx, 0)

    add_last_rows(0)
    add_own(0)
    for k in range(1, nz):
        if k < nz - 1:
            take_last(k)
        add_last_rows(k)
    def send_out(to):
        return pltpu.make_async_remote_copy(
            src_ref=attn.at[pl.ds(pl.multiple_of(to * tok, tok), tok)],
            dst_ref=out_ref.at[:, pl.ds(pl.multiple_of(s * head, head), head)],
            send_sem=osend, recv_sem=orecv,
            device_id={"sp": to}, device_id_type=MESH,
        )

    scale = head ** (-0.5) * log2e

    def attend(r, i, extent):
        at = pl.multiple_of((r * nx + i) * tok, tok)
        scores = lax.dot_general(
            qkv[pl.ds(at, tok), :head], qkv[:extent, head : 2 * head],
            (((1,), (1,)), ((), ())), preferred_element_type=jnp.float32,
        )
        offset = bias[pl.ds(at, tok), :extent] if kept else bias_of(at, tok, extent)
        scores = scores * scale + offset
        top = jnp.max(scores, axis=1, keepdims=True)
        weights = jnp.exp2(scores - top)
        total = jnp.sum(weights, axis=1, keepdims=True)
        summed = jnp.dot(
            weights.astype(jnp.bfloat16), qkv[:extent, 2 * head :],
            preferred_element_type=jnp.float32,
        )
        attn[pl.ds(at, tok), :] = (summed / total).astype(jnp.bfloat16)

    def attend_beside(r):
        def step(j):
            i = (x + j) % nx
            attend(r, i, (r + 1) * group)
            send_out(r * nx + i).start()

        if nx > 2:
            lax.fori_loop(1, nx, lambda j, carry: (step(j), carry)[1], 0)
        else:
            for j in range(1, nx):
                step(j)

    def attend_far(r):
        attend_beside(r)
        attend(r, x, (r + 1) * group)
        send_out(r * nx + x).start()

    def attend_before(r):
        if nx > 2:
            attend_far(r)
            return
        for i in range(nx):
            attend(r, i, (r * nx + i + 1) * tok)
            send_out(r * nx + i).start()

    def swapped():
        for k in range(1, ny):
            other = (y + k) % ny
            taken = qkv.at[pl.ds(pl.multiple_of(other * group, group), group)]
            pltpu.make_async_remote_copy(
                src_ref=taken, dst_ref=taken, send_sem=qsend.at[k - 1],
                recv_sem=qrecv.at[k - 1], device_id=aside(k), device_id_type=MESH,
            ).wait_recv()

    for j in range(1, nx):
        swap((x + j) % nx, 1)
    if nz > 1:
        take_last(nz - 1)
    for k in range(1, nz - 1):
        add_own(k)

    @pl.when(y > 0)
    def _():
        swapped()
        for r in range(ny - 1):
            pl.when(r < y)(lambda r=r: attend_before(r))

    if nz > 1:
        add_own(nz - 1)
    for i in range(nx):
        for g in range(2):
            qkv[own_rows(i, g), :] = acc[y, i, parts[g], :].astype(jnp.bfloat16)

    @pl.when(y == 0)
    def _():
        attend_beside(0)
        swapped()

    for r in range(1, ny):
        pl.when(r > y)(lambda r=r: attend_far(r))
    for r in range(1, ny):
        pl.when(y == r)(lambda r=r: attend_beside(r))
    for r in range(ny):
        pl.when(y == r)(lambda r=r: attend(r, x, (r + 1) * group))
    out_ref[:, pl.ds(pl.multiple_of(s * head, head), head)] = attn[
        pl.ds(pl.multiple_of(s * tok, tok), tok), :
    ]

    for j in range(1, nx):
        pltpu.make_async_remote_copy(
            src_ref=tok_hbm, dst_ref=xbuf.at[x], send_sem=xsend.at[j - 1],
            recv_sem=xrecv.at[j - 1, 0, 0],
            device_id={"sp": y * nx + (x + j) % nx}, device_id_type=MESH,
        ).wait_send()
    for zb in range(nz):
        upward = (z < nz - 1) & (zb <= z)
        downward = (z > 0) & (zb >= z)
        for h, part in [(y, whole)] + [(h, early_rows) for h in others]:
            pl.when(upward)(lambda: up(h, zb, part, 0).wait_send())
            pl.when(downward)(lambda: down(h, zb, part, 0).wait_send())
    if cores > 1:
        sent = wbuf.at[:, :, c]
        pltpu.make_async_remote_copy(
            src_ref=sent, dst_ref=sent, send_sem=psem, recv_sem=precv.at[0, 0],
            device_id=beside, device_id_type=MESH,
        ).wait_send()
    for k in range(1, ny):
        copy_block(
            y, z, c, early_rows, sideq.at[k - 1], farrecv.at[ny - k - 1, z, 0], aside(k)
        ).wait_send()
        sent = wbuf.at[y, :, c, late_rows]
        pltpu.make_async_remote_copy(
            src_ref=sent, dst_ref=sent, send_sem=sidesem.at[k - 1],
            recv_sem=farrecv.at[ny - k - 1, z, 0], device_id=aside(k), device_id_type=MESH,
        ).wait_send()
        pltpu.make_async_remote_copy(
            src_ref=qout.at[k - 1], dst_ref=qout.at[k - 1], send_sem=qsend.at[k - 1],
            recv_sem=qrecv.at[k - 1], device_id=aside(k), device_id_type=MESH,
        ).wait_send()
    rest = attn.at[pl.ds(0, length - tok)]
    ends = pltpu.make_async_remote_copy(
        src_ref=rest, dst_ref=rest, send_sem=osend, recv_sem=orecv,
        device_id={"sp": (s + 1) % (nx * ny)}, device_id_type=MESH,
    )
    ends.wait_recv()
    ends.wait_send()


def body(sp, dp, tokens, query_weight, key_weight, value_weight, cum_gate):
    nx = max(n for n in range(1, math.isqrt(sp) + 1) if sp % n == 0)
    ny = sp // nx
    cores = 2 if dp % 2 == 0 else 1
    nz = dp // cores
    tok, depth = tokens.shape[1:]
    rows, head = query_weight.shape
    length = sp * tok
    split = tok * 11 // 12 // 16 * 16
    early = rows * 11 // 32
    kept = length * length * 4 <= 8 * 1024 * 1024
    cuts = 3, 1
    dma = pltpu.SemaphoreType.DMA
    hbm = pl.BlockSpec(memory_space=pltpu.HBM)
    vmem = pl.BlockSpec(memory_space=pltpu.VMEM)
    out = pl.pallas_call(
        functools.partial(kernel, nx, ny, nz, cores, split, early, cuts, kept),
        out_shape=pltpu.VMEM((tok, sp * head), jnp.bfloat16),
        in_specs=[hbm] * 5,
        out_specs=vmem,
        scratch_shapes=[
            pltpu.VMEM((nx, tok, depth), jnp.bfloat16),
            pltpu.VMEM((ny, nz, cores, rows, 3 * head), jnp.bfloat16),
            pltpu.VMEM((ny, nx, tok, 3 * head), jnp.float32),
            pltpu.VMEM((length, 3 * head), jnp.bfloat16),
            pltpu.VMEM((ny - 1, nx, tok, 3 * head), jnp.bfloat16),
            pltpu.VMEM((1, length), jnp.float32),
            pltpu.VMEM((length, 128), jnp.float32),
            pltpu.VMEM((length, head), jnp.bfloat16),
            pltpu.VMEM((length, length) if kept else (8, 128), jnp.float32),
            dma,
            dma,
            dma,
            dma((nx - 1,)),
            dma((nx - 1, nz, 2)),
            dma((max(nz - 1, 1), sum(cuts))),
            dma((ny - 1, nz, cuts[1] + 1)),
            dma((ny, nz)),
            dma((ny, nz + 1)),
            dma((ny - 1,)),
            dma((ny - 1,)),
            dma,
            dma((ny - 1,)),
            dma((ny - 1,)),
            dma,
            dma,
        ],
        compiler_params=pltpu.CompilerParams(
            collective_id=0, has_side_effects=True, vmem_limit_bytes=60 * 1024 * 1024
        ),
    )(tokens[0], query_weight, key_weight, value_weight, cum_gate[0])
    return out[None]


def solution(mesh):
    in_specs = (
        P("dp", "sp", None),
        P("dp", "sp"),
        P("dp", "sp"),
        P("dp", "sp"),
        P("dp", "sp", None),
    )
    out_specs = P("dp", "sp", None)
    return jax.shard_map(
        functools.partial(body, mesh.shape["sp"], mesh.shape["dp"]),
        mesh=mesh, in_specs=in_specs, out_specs=out_specs, check_vma=False,
    )
```
